256 devices in a mesh: grp: 2 (over y), sp: 16 (over z), tp: 4 (over x), dp: 2 (over core).
Axes of the slice: x: 4, y: 2, z: 16, core: 2. Of those that a mesh axis runs over, the one named last changes fastest.
The devices are a block of a 4x16x16 slice.
Arguments:
- latent: bfloat16 [4, 10240, 2048], P(('grp', 'dp'), ('sp', 'tp')), parts along dimension 0, may hold values from -6 to 6
- cond: bfloat16 [4, 2048], P(('grp', 'dp'), 'sp'), parts along dimension 0, may hold values from -6 to 6
- cond_ctx: bfloat16 [2048], P('sp'), may hold values from -6 to 6
- context: bfloat16 [4, 512, 2048], P(('grp', 'dp'), 'sp'), parts along dimension 0, may hold values from -6 to 6
- w_mod: bfloat16 [3, 2048, 2048], P(None, 'sp', 'tp'), may hold values from -0.125 to 0.125
- norm_gain: float32 [2048], replicated, may hold values from 0.1 to 1.9
- w_query: bfloat16 [2048, 8, 128], P(None, 'tp'), may hold values from -5.347495 to 5.347495
- w_key: bfloat16 [2048, 8, 128], P(None, 'tp'), may hold values from -0.13258252 to 0.13258252
- w_value: bfloat16 [2048, 8, 128], P(None, 'tp'), may hold values from -0.125 to 0.125
- lam: float32 [8], P('tp'), may hold values from 0.3 to 0.8
- head_gain: float32 [128], replicated, may hold values from 0.1 to 1.9
- w_out: bfloat16 [8, 128, 2048], P('tp'), may hold values from -0.1875 to 0.1875
Outputs:
- updated: bfloat16 [4, 10240, 2048], P(('grp', 'dp'), ('sp', 'tp')), parts along dimension 0
The draws below stay inside these ranges and needn't reach their ends.
There are 2 independent parts, one for each index of `grp`. The reference program is written for one: setup_inputs(seed, part) draws one part's arguments, and reference() takes and returns one part's arrays. A program takes and returns all parts, laid end to end along the dimension named above; an argument that names none is the same for every part. Nothing has to cross between parts.
All inputs are finite; a program needn't handle non-finite values.
Results may differ from the reference program's by a relative error of at most 0.008.
Values may be sent and summed in bfloat16 or wider, within the bound.
A program may use at most 64 MiB of HBM per device.

```python
import math
import jax
import jax.numpy as jnp
from jax import lax

D = 2048
HEADS = 8
QK = 64
VD = 128
TOK_DEV = 640
CTX_DEV = 32
SAMPLES = 2
SEQ = 10240
CTX = 512
N_SP = 16


def key_base(key):
    drawn = jax.random.normal(jax.random.fold_in(key, 11), (D, HEADS, 2 * QK), jnp.float32)
    return jnp.clip(drawn, -6.0, 6.0) * D ** (-0.5)


def draw_w_key(key, part):
    return key_base(key).astype(jnp.bfloat16)


def draw_w_query(key, part):
    drawn = jax.random.normal(jax.random.fold_in(key, 12), (D, HEADS, 2 * QK), jnp.float32)
    fresh = jnp.clip(drawn, -6.0, 6.0) * (3.0 / D) ** 0.5
    return fresh.astype(jnp.bfloat16)


def block_scale(own_key, shape, pieces, low, top_value):
    def one(dim, blocks):
        heights = jax.random.uniform(jax.random.fold_in(jax.random.fold_in(own_key, 6), dim), (blocks,), jnp.float32, low / len(pieces), top_value / len(pieces))
        return jnp.repeat(jnp.exp(heights), shape[dim] // blocks).reshape((-1,) + (1,) * (len(shape) - dim - 1))

    loudness = one(*pieces[0])
    for cut in pieces[1:]:
        loudness = loudness * one(*cut)
    return loudness


def noise(rng, extent, spread, reach, cuts=(), held_as=jnp.bfloat16):
    values = jax.random.normal(rng, extent, jnp.float32) * spread
    if len(cuts) > 0:
        values = block_scale(rng, extent, cuts, -0.22, 0.18) * values
    return jnp.clip(values, min=-reach, max=reach).astype(held_as)


def setup_inputs(seed: int = 0, part: int = 0) -> dict:
    splits = jax.random.split(jax.random.key(seed), 13)
    part_splits = jax.random.split(jax.random.fold_in(splits[12], part), 13)
    return {
        "latent": noise(part_splits[0], (SAMPLES, SEQ, D), 1.0, 6.0, ((0, 2), (1, 64))),
        "cond": noise(part_splits[1], (SAMPLES, D), 1.0, 6.0, ((0, 2), (1, 16))),
        "cond_ctx": noise(splits[2], (D,), 1.0, 6.0, ((0, 16),)),
        "context": noise(part_splits[3], (SAMPLES, CTX, D), 1.0, 6.0, ((0, 2), (1, 16))),
        "w_mod": noise(splits[4], (3, D, D), D ** -0.5, 0.125, ((1, 16), (2, 4))),
        "norm_gain": jnp.clip(1.0 + 0.18 * jax.random.normal(splits[5], (D,), jnp.float32), 0.1, 1.9),
        "w_query": draw_w_query(jax.random.fold_in(splits[12], 71), part),
        "w_key": draw_w_key(jax.random.fold_in(splits[12], 71), part),
        "w_value": noise(splits[8], (D, HEADS, VD), D ** -0.5, 0.125, ((1, 4),)),
        "lam": jnp.clip(0.3 + 0.5 * jax.random.uniform(splits[9], (HEADS,), jnp.float32) ** block_scale(splits[9], (HEADS,), ((0, 4),), -0.2, 0.2), 0.3, 0.8),
        "head_gain": jnp.clip(1.0 + 0.18 * jax.random.normal(splits[10], (VD,), jnp.float32), 0.1, 1.9),
        "w_out": noise(splits[11], (HEADS, VD, D), (HEADS * VD) ** -0.5, 0.1875, ((0, 4),)),
    }


EPSILON = 1e-06
HEAD_SCALE = 0.8

def modulated_norm(tokens, norm_gain, shift, scale):
    values_f = tokens.astype(jnp.float32)
    normed = values_f * lax.rsqrt(lax.optimization_barrier(jnp.mean(values_f * values_f, axis=-1, keepdims=True)) + EPSILON)
    return (normed * norm_gain * (1.0 + scale) + shift).astype(jnp.bfloat16)

def project_weight(tokens, weight):
    flat_weight = weight.reshape(weight.shape[0], weight.shape[1] * weight.shape[2])
    product = jnp.dot(tokens, flat_weight, preferred_element_type=jnp.float32).astype(jnp.bfloat16)
    return product.reshape(tokens.shape[0], weight.shape[1], weight.shape[2])

def attend_rows(queries, keys, values, key_lift, lam, head_gain):
    map_outs = []
    for which_map in range(2):
        first_col = which_map * QK
        scores = jnp.einsum('qhd,khd->qhk', queries[..., first_col:first_col + QK].astype(jnp.float32), keys[..., first_col:first_col + QK].astype(jnp.float32)) * QK ** (-0.5) + key_lift
        highest = lax.optimization_barrier(jnp.max(scores, axis=-1, keepdims=True))
        weights = jnp.exp(scores - highest)
        totals = lax.optimization_barrier(jnp.sum(weights, axis=-1))
        rounded = lax.optimization_barrier(weights.astype(jnp.bfloat16)).astype(jnp.float32)
        summed = jnp.einsum('qhk,khd->qhd', rounded, values.astype(jnp.float32))
        map_outs.append(summed / totals[..., None])
    differ = map_outs[0] - lam[None, :, None] * map_outs[1]
    normed = differ * lax.rsqrt(lax.optimization_barrier(jnp.mean(differ * differ, axis=-1, keepdims=True)) + EPSILON)
    return (normed * head_gain * HEAD_SCALE).astype(jnp.bfloat16)

def reference(latent, cond, cond_ctx, context, w_mod, norm_gain, w_query, w_key, w_value, lam, head_gain, w_out):
    lift_value = math.log(TOK_DEV / (4 * CTX_DEV))
    cond_rows = jnp.concatenate([cond.astype(jnp.float32), cond_ctx.astype(jnp.float32)[None]], axis=0)
    modulation = jnp.einsum('sd,jde->sje', jax.nn.silu(cond_rows), w_mod.astype(jnp.float32), precision=lax.Precision.HIGHEST)
    ctx_mod = modulation[SAMPLES]
    key_lift = jnp.concatenate([jnp.zeros((SEQ,), jnp.float32), jnp.full((CTX,), lift_value, jnp.float32)])
    results = []
    for sample in range(SAMPLES):
        sample_mod = modulation[sample]
        normed = modulated_norm(latent[sample], norm_gain, sample_mod[0], sample_mod[1])
        ctx_normed = modulated_norm(context[sample], norm_gain, ctx_mod[0], ctx_mod[1])
        queries = project_weight(normed, w_query)
        keys = jnp.concatenate([project_weight(normed, w_key), project_weight(ctx_normed, w_key)], axis=0)
        values = jnp.concatenate([project_weight(normed, w_value), project_weight(ctx_normed, w_value)], axis=0)
        query_blocks = queries.reshape(N_SP, TOK_DEV, HEADS, 2 * QK)
        attended = lax.map(lambda block: attend_rows(block, keys, values, key_lift, lam, head_gain), query_blocks)
        flat_heads = attended.reshape(SEQ, HEADS * VD)
        mixed = jnp.dot(flat_heads, w_out.reshape(HEADS * VD, D), preferred_element_type=jnp.float32)
        results.append((latent[sample].astype(jnp.float32) + sample_mod[2] * mixed).astype(jnp.bfloat16))
    return jnp.stack(results)
```

```python
import functools
import math

import jax
import jax.numpy as jnp
from jax import lax
from jax.experimental import pallas as pl
from jax.experimental.pallas import tpu as pltpu
from jax.sharding import PartitionSpec as P

TOK_DEV = 640
CTX_DEV = 32

EPSILON = 1e-06
HEAD_SCALE = 0.8
MESH = pl.DeviceIdType.MESH
QTILE = 256


def remote(src, dst, send, recv, device):
    return pltpu.make_async_remote_copy(
        src_ref=src,
        dst_ref=dst,
        send_sem=send,
        recv_sem=recv,
        device_id=device,
        device_id_type=MESH,
    )


def greet(peers):
    barrier = pltpu.get_barrier_semaphore()
    for peer in peers:
        pl.semaphore_signal(barrier, inc=1, device_id=peer, device_id_type=MESH)
    pl.semaphore_wait(barrier, len(peers))


def exchange_kernel(
    n_sp, n_tp, part, latent, mod, rows, far, near, total, far_s, far_r, near_s, near_r, tp_s, tp_r, lat_s, lat_r, own_s
):
    z = lax.axis_index("sp")
    x = lax.axis_index("tp")
    quarter = n_sp // 4

    def sp_at(offset):
        return {"sp": lax.rem(z + offset + n_sp, n_sp)}

    def tp_at(offset):
        return {"tp": lax.rem(x + offset, n_tp)}

    far_peers = [sp_at(quarter * k) for k in (1, 2, 3)]
    near_peers = [sp_at(1), sp_at(-1), sp_at(2)]
    tp_peers = [tp_at(k) for k in (1, 2, 3)]
    greet(far_peers + near_peers + [sp_at(-2)] + tp_peers)
    right, left = tp_at(1), tp_at(n_tp - 1)
    half = latent.shape[0] // 2
    first, second = pl.ds(0, half), pl.ds(half, half)

    own = pltpu.make_async_copy(latent, rows.at[0], own_s)
    far_copies = [
        remote(part, far.at[k], far_s.at[k], far_r.at[k], far_peers[k]) for k in range(3)
    ]
    for copy in far_copies:
        copy.start()
    to_right = [
        remote(latent.at[part_rows], rows.at[1, part_rows], lat_s.at[k], lat_r.at[k], right)
        for k, part_rows in enumerate((first, second))
    ]
    to_left = [
        remote(latent.at[part_rows], rows.at[2, part_rows], lat_s.at[2 + k], lat_r.at[2 + k], left)
        for k, part_rows in enumerate((second, first))
    ]
    to_right[0].start()
    to_left[0].start()
    to_right[1].start()
    to_left[1].start()
    own.start()
    for copy in far_copies:
        copy.wait_recv()
    total[...] = part[...] + far[0] + far[1] + far[2]
    near_copies = [
        remote(total, near.at[k], near_s.at[k], near_r.at[k], near_peers[k]) for k in range(3)
    ]
    for copy in near_copies:
        copy.start()
    to_right[0].wait_recv()
    onward_right = remote(
        rows.at[1, first], rows.at[3, first], lat_s.at[4], lat_r.at[4], right
    )
    onward_right.start()
    to_left[0].wait_recv()
    onward_left = remote(
        rows.at[2, second], rows.at[3, second], lat_s.at[5], lat_r.at[5], left
    )
    onward_left.start()
    for copy in near_copies:
        copy.wait_recv()
    columns = part.shape[1]
    mine = pl.ds(pl.multiple_of(x * columns, columns), columns)
    mod[:, mine] = total[...] + near[0] + near[1] + near[2]
    tp_copies = [
        remote(mod.at[:, mine], mod.at[:, mine], tp_s.at[k], tp_r.at[k], tp_peers[k])
        for k in range(3)
    ]
    for copy in tp_copies:
        copy.start()
    for k in range(3):
        source = lax.rem(x + n_tp - 1 - k, n_tp)
        theirs = pl.ds(pl.multiple_of(source * columns, columns), columns)
        remote(mod.at[:, theirs], mod.at[:, theirs], tp_s.at[k], tp_r.at[k], tp_peers[k]).wait_recv()
    to_right[1].wait_recv()
    to_left[1].wait_recv()
    onward_right.wait_recv()
    onward_left.wait_recv()
    own.wait()
    for copy in far_copies + near_copies + tp_copies + to_right + to_left + [onward_right, onward_left]:
        copy.wait_send()


def exchange(n_sp, n_tp, part, latent):
    dma = pltpu.SemaphoreType.DMA
    vmem = pl.BlockSpec(memory_space=pltpu.VMEM)
    return pl.pallas_call(
        functools.partial(exchange_kernel, n_sp, n_tp),
        out_shape=(
            jax.ShapeDtypeStruct((part.shape[0], part.shape[1] * n_tp), jnp.float32),
            jax.ShapeDtypeStruct((n_tp,) + latent.shape, latent.dtype),
        ),
        in_specs=[vmem] * 2,
        out_specs=(vmem, vmem),
        scratch_shapes=[
            pltpu.VMEM((3,) + part.shape, jnp.float32),
            pltpu.VMEM((3,) + part.shape, jnp.float32),
            pltpu.VMEM(part.shape, jnp.float32),
            dma((3,)),
            dma((3,)),
            dma((3,)),
            dma((3,)),
            dma((3,)),
            dma((3,)),
            dma((6,)),
            dma((6,)),
            dma,
        ],
        compiler_params=pltpu.CompilerParams(collective_id=0, has_side_effects=True),
        name="exchange",
    )(part, latent)


def attend_kernel(
    n_sp, n_tp, n_ctx, lift, kv, q_t, lam, head_gain, w_out, latent, gate, out,
    blocks, w_far, q_wide, acc, top, total, v_t, att, got,
    own_s, ring_s, ring_r, w_s, w_r, att_s, att_r,
):
    z = lax.axis_index("sp")
    x = lax.axis_index("tp")
    length = kv.shape[0]
    chunk = length // 2
    heads = lam.shape[0]
    width = head_gain.shape[0]
    n_query = q_t.shape[1]
    tiles = 2 * n_query // QTILE
    last = n_sp - 2

    def sp_to(direction):
        return {"sp": lax.rem(z + 1 - 2 * direction + n_sp, n_sp)}

    def tp_at(offset):
        return {"tp": lax.rem(x + offset, n_tp)}

    tp_peers = [tp_at(k) for k in (1, 2, 3)]
    greet([sp_to(0), sp_to(1)] + tp_peers)
    right, left = tp_peers[0], tp_peers[2]

    own_copies = []
    for c in range(2):
        for d in range(2):
            span = pl.ds(c * chunk, chunk)
            own_copies.append(
                remote(kv.at[span], blocks.at[d, span], own_s.at[d, c], ring_r.at[d, c], sp_to(d))
            )
    for copy in own_copies:
        copy.start()
    w_rows = w_out.shape[0]
    upper, lower = pl.ds(0, w_rows // 2), pl.ds(w_rows // 2, w_rows // 2)
    w_right = remote(w_out, w_far.at[0], w_s.at[0], w_r.at[0], right)
    w_left = remote(w_out, w_far.at[2], w_s.at[1], w_r.at[1], left)
    w_right_on = remote(w_far.at[0, upper], w_far.at[1, upper], w_s.at[2], w_r.at[2], right)
    w_left_on = remote(w_far.at[2, lower], w_far.at[1, lower], w_s.at[3], w_r.at[3], left)
    w_right.start()
    w_left.start()

    q_wide[...] = jnp.zeros_like(q_wide)
    half_width = width // 2
    for h in range(heads):
        for m in range(2):
            span = slice(h * width + m * half_width, h * width + (m + 1) * half_width)
            q_wide[span, m * n_query : (m + 1) * n_query] = q_t[span, :]
    acc[...] = jnp.zeros_like(acc)
    total[...] = jnp.zeros_like(total)
    top[...] = jnp.full_like(top, -1e30)

    def fold(block):
        def head(h, carry):
            base = pl.multiple_of(h * width, width)
            keys = block[:, pl.ds(base, width)]
            v_t[...] = block[:, pl.ds(pl.multiple_of(heads * width + base, width), width)].T
            for j in range(tiles):
                columns = slice(j * QTILE, (j + 1) * QTILE)
                scores = jnp.dot(
                    keys, q_wide[pl.ds(base, width), columns], preferred_element_type=jnp.float32
                )
                scores = jnp.concatenate(
                    [scores[: length - n_ctx], scores[length - n_ctx :] + lift], axis=0
                )
                old = top[h, :, columns]
                new = jnp.maximum(old, jnp.max(scores, axis=0, keepdims=True))
                weights = jnp.exp(scores - new)
                rescale = jnp.exp(old - new)
                top[h, :, columns] = new
                total[h, :, columns] = total[h, :, columns] * rescale + jnp.sum(
                    weights, axis=0, keepdims=True
                )
                acc[h, :, columns] = acc[h, :, columns] * rescale + jnp.dot(
                    v_t[...], weights.astype(jnp.bfloat16), preferred_element_type=jnp.float32
                )
            return carry

        lax.fori_loop(0, heads, head, 0)

    def ring_copy(t, c):
        span = pl.ds(c * chunk, chunk)
        target = jnp.minimum(t + 2, last)
        return remote(
            blocks.at[t, span],
            blocks.at[target, span],
            ring_s.at[t, c],
            ring_r.at[target, c],
            sp_to(lax.rem(t, 2)),
        )

    def arrival(t, c):
        span = pl.ds(c * chunk, chunk)
        return remote(
            blocks.at[t, span], blocks.at[t, span], ring_s.at[t, c], ring_r.at[t, c], sp_to(0)
        )

    def forwards(t, c):
        return jnp.logical_or(t < last - 2, t == last - 2 + c)

    fold(kv)

    def ring_step(t, carry):
        for c in range(2):
            arrival(t, c).wait_recv()

            @pl.when(forwards(t, c))
            def _():
                ring_copy(t, c).start()

        @pl.when(t == 6)
        def _():
            w_right.wait_recv()
            w_right_on.start()
            w_left.wait_recv()
            w_left_on.start()

        fold(blocks.at[t])
        return carry

    lax.fori_loop(0, last + 1, ring_step, 0)

    for h in range(heads):
        first = acc[h, :, :n_query] / total[h, :, :n_query]
        second = acc[h, :, n_query:] / total[h, :, n_query:]
        differ = first - lam[h] * second
        scale = lax.rsqrt(jnp.mean(differ * differ, axis=0, keepdims=True) + EPSILON)
        normed = differ * scale * head_gain[...] * HEAD_SCALE
        att[:, h * width : (h + 1) * width] = normed.T.astype(jnp.bfloat16)

    own_rows = latent.shape[0]
    slot_of = {1: 2, 2: 3, 3: 1}
    sends = []
    for k in (1, 2, 3):
        sends.append(
            remote(
                att.at[pl.ds(slot_of[k] * own_rows, own_rows)],
                got.at[k - 1],
                att_s.at[k - 1],
                att_r.at[k - 1],
                tp_peers[k - 1],
            )
        )
    for copy in sends:
        copy.start()
    w_right_on.wait_recv()
    w_left_on.wait_recv()
    for copy in sends:
        copy.wait_recv()
    n_columns = latent.shape[1]
    step = 512
    for j in range(n_columns // step):
        columns = slice(j * step, (j + 1) * step)
        mixed = jnp.dot(att[:own_rows, :], w_out[:, columns], preferred_element_type=jnp.float32)
        for k in range(3):
            mixed += jnp.dot(got[k], w_far[k, :, columns], preferred_element_type=jnp.float32)
        out[:, columns] = (
            latent[:, columns].astype(jnp.float32) + gate[:, columns] * mixed
        ).astype(out.dtype)

    for copy in own_copies + [w_right, w_left, w_right_on, w_left_on] + sends:
        copy.wait_send()

    def drain(t, carry):
        for c in range(2):

            @pl.when(forwards(t, c))
            def _():
                ring_copy(t, c).wait_send()

        return carry

    lax.fori_loop(0, last + 1, drain, 0)


def attend(n_sp, n_tp, n_ctx, lift, kv, q_t, lam, head_gain, w_out, latent, gate):
    dma = pltpu.SemaphoreType.DMA
    vmem = pl.BlockSpec(memory_space=pltpu.VMEM)
    heads, width, n_query = lam.shape[0], head_gain.shape[0], q_t.shape[1]
    length = kv.shape[0]
    return pl.pallas_call(
        functools.partial(attend_kernel, n_sp, n_tp, n_ctx, lift),
        out_shape=jax.ShapeDtypeStruct(latent.shape, latent.dtype),
        in_specs=[vmem, vmem, pl.BlockSpec(memory_space=pltpu.SMEM)] + [vmem] * 4,
        out_specs=vmem,
        scratch_shapes=[
            pltpu.VMEM((n_sp - 1,) + kv.shape, kv.dtype),
            pltpu.VMEM((3,) + w_out.shape, w_out.dtype),
            pltpu.VMEM((heads * width, 2 * n_query), jnp.bfloat16),
            pltpu.VMEM((heads, width, 2 * n_query), jnp.float32),
            pltpu.VMEM((heads, 1, 2 * n_query), jnp.float32),
            pltpu.VMEM((heads, 1, 2 * n_query), jnp.float32),
            pltpu.VMEM((width, length), jnp.bfloat16),
            pltpu.VMEM((n_query, heads * width), jnp.bfloat16),
            pltpu.VMEM((3, latent.shape[0], heads * width), jnp.bfloat16),
            dma((2, 2)),
            dma((n_sp - 1, 2)),
            dma((n_sp - 1, 2)),
            dma((4,)),
            dma((4,)),
            dma((3,)),
            dma((3,)),
        ],
        compiler_params=pltpu.CompilerParams(
            collective_id=1, has_side_effects=True, vmem_limit_bytes=56 * 1024 * 1024
        ),
        name="attend",
    )(kv, q_t, lam, head_gain, w_out, latent, gate)


def modulated_norm(tokens, norm_gain, shift, scale):
    values_f = tokens.astype(jnp.float32)
    normed = values_f * lax.rsqrt(jnp.mean(values_f * values_f, axis=-1, keepdims=True) + EPSILON)
    return (normed * norm_gain * (1.0 + scale) + shift).astype(jnp.bfloat16)


def flat(weight):
    return weight.reshape(weight.shape[0], weight.shape[1] * weight.shape[2])


def on_device(
    latent, cond, cond_ctx, context, w_mod, norm_gain, w_query, w_key, w_value, lam, head_gain, w_out
):
    n_sp, n_tp = lax.axis_size("sp"), lax.axis_size("tp")
    lift = math.log(TOK_DEV / (4 * CTX_DEV))
    cond_rows = jnp.concatenate(
        [cond.astype(jnp.float32), cond_ctx.astype(jnp.float32)[None]], axis=0
    )
    partial_mod = jnp.einsum(
        "sd,jde->sje",
        jax.nn.silu(cond_rows),
        w_mod.astype(jnp.float32),
        precision=lax.Precision.HIGHEST,
    )
    columns = w_mod.shape[2]
    part = jnp.concatenate(
        [partial_mod.reshape(6, columns), jnp.zeros((2, columns), jnp.float32)], axis=0
    )
    modulation, rows = exchange(n_sp, n_tp, part, latent[0])
    rows = rows.reshape(-1, rows.shape[2])
    normed = modulated_norm(rows, norm_gain, modulation[0], modulation[1])
    ctx_normed = modulated_norm(context[0], norm_gain, modulation[3], modulation[4])
    tokens = jnp.concatenate([normed, ctx_normed], axis=0)
    keys = jnp.dot(tokens, flat(w_key), preferred_element_type=jnp.float32)
    values = jnp.dot(tokens, flat(w_value), preferred_element_type=jnp.float32)
    kv = jnp.concatenate([keys.astype(jnp.bfloat16), values.astype(jnp.bfloat16)], axis=1)
    half = w_query.shape[2] // 2
    q_t = lax.dot_general(
        flat(w_query), normed, (((0,), (1,)), ((), ())), preferred_element_type=jnp.float32
    )
    q_t = q_t.astype(jnp.bfloat16) * jnp.bfloat16(half ** (-0.5))
    updated = attend(
        n_sp,
        n_tp,
        context.shape[1],
        lift,
        kv,
        q_t,
        lam,
        head_gain[:, None],
        w_out.reshape(-1, w_out.shape[2]),
        latent[0],
        modulation[2:3],
    )
    return updated[None]


def solution(mesh):
    return jax.shard_map(
        on_device,
        mesh=mesh,
        in_specs=(
            P(("grp", "dp"), ("sp", "tp"), None),
            P(("grp", "dp"), "sp"),
            P("sp"),
            P(("grp", "dp"), "sp", None),
            P(None, "sp", "tp"),
            P(),
            P(None, "tp", None),
            P(None, "tp", None),
            P(None, "tp", None),
            P("tp"),
            P(),
            P("tp", None, None),
        ),
        out_specs=P(("grp", "dp"), ("sp", "tp"), None),
        check_vma=False,
    )
```

```python
import functools
import math

import jax
import jax.numpy as jnp
from jax import lax
from jax.experimental import pallas as pl
from jax.experimental.pallas import tpu as pltpu
from jax.sharding import PartitionSpec as P

TOK_DEV = 640
CTX_DEV = 32

EPSILON = 1e-06
HEAD_SCALE = 0.8
MESH = pl.DeviceIdType.MESH
QTILE = 256


def remote(src, dst, send, recv, device):
    return pltpu.make_async_remote_copy(
        src_ref=src,
        dst_ref=dst,
        send_sem=send,
        recv_sem=recv,
        device_id=device,
        device_id_type=MESH,
    )


def greet(peers):
    barrier = pltpu.get_barrier_semaphore()
    for peer in peers:
        pl.semaphore_signal(barrier, inc=1, device_id=peer, device_id_type=MESH)
    pl.semaphore_wait(barrier, len(peers))


def fused_kernel(
    n_sp, n_tp, lift,
    part, latent, context, norm_gain, w_query, w_key, w_value, lam, head_gain, w_out, out,
    far, near, sums, mod, rows, w_raw, w_kv, w_q, w_own, w_far, tokens, queries,
    blocks, q_wide, acc, top, total, v_t, att, got,
    far_s, far_r, near_s, near_r, tp_s, tp_r, lat_s, lat_r, load_s, ring_s, ring_r, w_s, w_r, att_s, att_r,
):
    z = lax.axis_index("sp")
    x = lax.axis_index("tp")
    own_rows, n_ctx = latent.shape[0], context.shape[0]
    heads = lam.shape[0]
    width = head_gain.shape[0]
    n_query = n_tp * own_rows
    length = n_query + n_ctx
    tiles = 2 * n_query // QTILE
    steps = n_sp // 2
    starts = [0] + [n_ctx + k * own_rows for k in range(1, n_tp)]
    sizes = [n_ctx + own_rows] + [own_rows] * (n_tp - 1)

    def sp_at(offset):
        return {"sp": lax.rem(z + offset + n_sp, n_sp)}

    def tp_at(offset):
        return {"tp": lax.rem(x + offset, n_tp)}

    quarter = n_sp // 4
    far_peers = [sp_at(quarter * k) for k in (1, 2, 3)]
    near_peers = [sp_at(1), sp_at(-1), sp_at(2)]
    tp_peers = [tp_at(k) for k in (1, 2, 3)]
    right, left = tp_peers[0], tp_peers[2]
    ring_peers = [sp_at(1), sp_at(-1)]

    raw = [w_key, w_value, w_query]
    raw_loads = [pltpu.make_async_copy(raw[k], w_raw.at[k], load_s.at[k]) for k in range(3)]
    out_load = pltpu.make_async_copy(w_out, w_own, load_s.at[3])
    for copy in raw_loads + [out_load]:
        copy.start()
    greet(far_peers + near_peers + [sp_at(-2)] + tp_peers)

    far_copies = [
        remote(part, far.at[k], far_s.at[k], far_r.at[k], far_peers[k]) for k in range(3)
    ]
    for copy in far_copies:
        copy.start()

    half = own_rows // 2
    piece = 48

    def send_rows(k, slot, first, count, peer):
        span = pl.ds(first, count)
        return remote(latent.at[span], rows.at[slot, span], lat_s.at[k], lat_r.at[k], peer)

    to_right = [
        send_rows(0, 0, 0, half, right),
        send_rows(1, 0, half, piece, right),
        send_rows(2, 0, half + piece, half - piece, right),
    ]
    to_left = [
        send_rows(3, 1, half, half, left),
        send_rows(4, 1, 0, piece, left),
        send_rows(5, 1, piece, half - piece, left),
    ]
    first, second = pl.ds(0, half), pl.ds(half, half)
    onward_right = remote(rows.at[0, first], rows.at[2, first], lat_s.at[6], lat_r.at[6], right)
    onward_left = remote(rows.at[1, second], rows.at[2, second], lat_s.at[7], lat_r.at[7], left)
    for k in range(2):
        to_right[k].start()
        to_left[k].start()

    q_wide[...] = jnp.zeros_like(q_wide)
    acc[...] = jnp.zeros_like(acc)
    total[...] = jnp.zeros_like(total)
    top[...] = jnp.full_like(top, -1e30)
    for k in range(2):
        raw_loads[k].wait()
        for h in range(heads):
            column = (k * heads + h) * width
            w_kv[:, column : column + width] = w_raw[k, :, h, :]

    for copy in far_copies:
        copy.wait_recv()
    sums[...] = part[...] + far[0] + far[1] + far[2]
    near_copies = [
        remote(sums, near.at[k], near_s.at[k], near_r.at[k], near_peers[k]) for k in range(3)
    ]
    for copy in near_copies:
        copy.start()
    raw_loads[2].wait()
    for h in range(heads):
        w_q[:, h * width : (h + 1) * width] = w_raw[2, :, h, :]
    for copy in near_copies:
        copy.wait_recv()
    columns = part.shape[1]

    def mod_of(owner):
        span = pl.ds(pl.multiple_of(owner * columns, columns), columns)
        return mod.at[:, span]

    mine = pl.ds(pl.multiple_of(x * columns, columns), columns)
    mod[:, mine] = sums[...] + near[0] + near[1] + near[2]
    tp_copies = [
        remote(mod_of(x), mod_of(x), tp_s.at[k], tp_r.at[k], tp_peers[k]) for k in range(3)
    ]
    for copy in tp_copies:
        copy.start()
    to_right[2].start()
    to_left[2].start()
    to_right[0].wait_recv()
    onward_right.start()
    to_left[0].wait_recv()
    onward_left.start()
    for k in range(3):
        theirs = mod_of(lax.rem(x + n_tp - 1 - k, n_tp))
        remote(theirs, theirs, tp_s.at[k], tp_r.at[k], tp_peers[k]).wait_recv()

    def norm(source, target, count, kind):
        gain = norm_gain[...] * (1.0 + mod[kind + 1 : kind + 2, :])
        shift = mod[kind : kind + 1, :]
        group = 16

        def some(i, carry):
            span = pl.ds(pl.multiple_of(i * group, group), group)
            values = source[span, :].astype(jnp.float32)
            scale = lax.rsqrt(jnp.mean(values * values, axis=-1, keepdims=True) + EPSILON)
            spot = pl.ds(pl.multiple_of(target + i * group, group), group)
            tokens[spot, :] = (values * scale * gain + shift).astype(jnp.bfloat16)
            return carry

        lax.fori_loop(0, count // group, some, 0, unroll=2)

    def ring_copy(slot, target, d, c):
        span = pl.ds(starts[c], sizes[c])
        return remote(
            blocks.at[slot, span],
            blocks.at[target, span],
            ring_s.at[slot, d, c],
            ring_r.at[target, c],
            ring_peers[d],
        )

    def project(c):
        span = slice(starts[c], starts[c] + sizes[c])
        blocks[0, span, :] = jnp.dot(
            tokens[: sizes[c], :], w_kv[...], preferred_element_type=jnp.float32
        ).astype(jnp.bfloat16)
        queries[c * own_rows : (c + 1) * own_rows, :] = jnp.dot(
            tokens[:own_rows, :], w_q[...], preferred_element_type=jnp.float32
        ).astype(jnp.bfloat16)
        for d in range(2):
            ring_copy(0, 1 + d, d, c).start()

    norm(latent, 0, own_rows, 0)
    norm(context, own_rows, n_ctx, 3)
    project(0)
    for k in (1, 2):
        to_right[k].wait_recv()
    norm(rows.at[0], 0, own_rows, 0)
    project(1)
    for k in (1, 2):
        to_left[k].wait_recv()
    norm(rows.at[1], 0, own_rows, 0)
    project(2)
    onward_right.wait_recv()
    onward_left.wait_recv()
    norm(rows.at[2], 0, own_rows, 0)
    project(3)

    w_rows = w_own.shape[0]
    upper, lower = pl.ds(0, w_rows // 2), pl.ds(w_rows // 2, w_rows // 2)
    w_right = remote(w_own, w_far.at[0], w_s.at[0], w_r.at[0], right)
    w_left = remote(w_own, w_far.at[2], w_s.at[1], w_r.at[1], left)
    w_right_on = remote(w_far.at[0, upper], w_far.at[1, upper], w_s.at[2], w_r.at[2], right)
    w_left_on = remote(w_far.at[2, lower], w_far.at[1, lower], w_s.at[3], w_r.at[3], left)
    out_load.wait()
    w_right.start()
    w_left.start()

    half_width = width // 2
    for h in range(heads):
        for m in range(2):
            span = slice(h * width + m * half_width, h * width + (m + 1) * half_width)
            q_wide[span, m * n_query : (m + 1) * n_query] = queries[:, span].T * jnp.bfloat16(
                half_width ** (-0.5)
            )

    def fold(block):
        def head(h, carry):
            base = pl.multiple_of(h * width, width)
            keys = block[:, pl.ds(base, width)]
            v_t[...] = block[:, pl.ds(pl.multiple_of(heads * width + base, width), width)].T
            for j in range(tiles):
                columns = slice(j * QTILE, (j + 1) * QTILE)
                scores = jnp.dot(
                    keys, q_wide[pl.ds(base, width), columns], preferred_element_type=jnp.float32
                )
                scores = jnp.concatenate(
                    [
                        scores[:own_rows],
                        scores[own_rows : own_rows + n_ctx] + lift,
                        scores[own_rows + n_ctx :],
                    ],
                    axis=0,
                )
                old = top[h, :, columns]
                new = jnp.maximum(old, jnp.max(scores, axis=0, keepdims=True))
                weights = jnp.exp(scores - new)
                rescale = jnp.exp(old - new)
                top[h, :, columns] = new
                total[h, :, columns] = total[h, :, columns] * rescale + jnp.sum(
                    weights, axis=0, keepdims=True
                )
                acc[h, :, columns] = acc[h, :, columns] * rescale + jnp.dot(
                    v_t[...], weights.astype(jnp.bfloat16), preferred_element_type=jnp.float32
                )
            return carry

        lax.fori_loop(0, heads, head, 0)

    def forward(s, d, c):
        slot = 2 * s - 1 + d
        return ring_copy(slot, jnp.minimum(slot + 2, 2 * steps - 1), d, c)

    def arrived(slot, c):
        ring_copy(slot, slot, 0, c).wait_recv()

    def always(d, c):
        return (c < n_tp // 2) == (d == 0)

    def half_step(u, carry):
        s = u // 2 + 1
        for phase in range(2):

            @pl.when(jnp.logical_and(u < 2 * steps - 2, u % 2 == phase))
            def _():
                for c in (2 * phase, 2 * phase + 1):
                    for d in range(2):
                        arrived(2 * s - 1 + d, c)
                        if always(d, c):
                            forward(s, d, c).start()
                        else:

                            @pl.when(s < steps - 1)
                            def _():
                                forward(s, d, c).start()

            @pl.when(u == 2 * steps - 2 + phase)
            def _():
                arrived(2 * steps - 1, phase)
                arrived(2 * steps - 1, 2 + phase)

        @pl.when(u == 6)
        def _():
            w_right.wait_recv()
            w_right_on.start()
            w_left.wait_recv()
            w_left_on.start()

        fold(blocks.at[u])
        return carry

    lax.fori_loop(0, 2 * steps, half_step, 0)

    for h in range(heads):
        one = acc[h, :, :n_query] / total[h, :, :n_query]
        two = acc[h, :, n_query:] / total[h, :, n_query:]
        differ = one - lam[h] * two
        scale = lax.rsqrt(jnp.mean(differ * differ, axis=0, keepdims=True) + EPSILON)
        normed = differ * scale * head_gain[...] * HEAD_SCALE
        att[:, h * width : (h + 1) * width] = normed.T.astype(jnp.bfloat16)

    slot_of = {1: 2, 2: 3, 3: 1}
    sends = []
    for k in (1, 2, 3):
        span = pl.ds(slot_of[k] * own_rows, own_rows)
        sends.append(
            remote(att.at[span], got.at[k - 1], att_s.at[k - 1], att_r.at[k - 1], tp_peers[k - 1])
        )
    for copy in sends:
        copy.start()
    w_right_on.wait_recv()
    w_left_on.wait_recv()
    for copy in sends:
        copy.wait_recv()
    n_columns = latent.shape[1]
    step = 512
    for j in range(n_columns // step):
        columns = slice(j * step, (j + 1) * step)
        mixed = jnp.dot(att[:own_rows, :], w_own[:, columns], preferred_element_type=jnp.float32)
        for k in range(3):
            mixed += jnp.dot(got[k], w_far[k, :, columns], preferred_element_type=jnp.float32)
        out[:, columns] = (
            latent[:, columns].astype(jnp.float32) + mod[2:3, columns] * mixed
        ).astype(out.dtype)

    for copy in far_copies + near_copies + tp_copies + to_right + to_left + sends:
        copy.wait_send()
    for copy in [onward_right, onward_left, w_right, w_left, w_right_on, w_left_on]:
        copy.wait_send()
    for c in range(n_tp):
        for d in range(2):
            ring_copy(0, 1 + d, d, c).wait_send()

    def drain(s, carry):
        for c in range(n_tp):
            for d in range(2):
                if always(d, c):
                    forward(s, d, c).wait_send()
                else:

                    @pl.when(s < steps - 1)
                    def _():
                        forward(s, d, c).wait_send()

        return carry

    lax.fori_loop(1, steps, drain, 0)


def fused(n_sp, n_tp, lift, part, latent, context, norm_gain, w_query, w_key, w_value, lam, head_gain, w_out):
    dma = pltpu.SemaphoreType.DMA
    vmem = pl.BlockSpec(memory_space=pltpu.VMEM)
    anywhere = pl.BlockSpec(memory_space=pl.ANY)
    heads, width = lam.shape[0], head_gain.shape[0]
    own_rows, model = latent.shape
    n_query = n_tp * own_rows
    length = n_query + context.shape[0]
    bf16, f32 = jnp.bfloat16, jnp.float32
    return pl.pallas_call(
        functools.partial(fused_kernel, n_sp, n_tp, lift),
        out_shape=jax.ShapeDtypeStruct(latent.shape, latent.dtype),
        in_specs=[vmem] * 4
        + [anywhere] * 3
        + [pl.BlockSpec(memory_space=pltpu.SMEM), vmem, anywhere],
        out_specs=vmem,
        scratch_shapes=[
            pltpu.VMEM((3,) + part.shape, f32),
            pltpu.VMEM((3,) + part.shape, f32),
            pltpu.VMEM(part.shape, f32),
            pltpu.VMEM((part.shape[0], model), f32),
            pltpu.VMEM((3, own_rows, model), bf16),
            pltpu.VMEM((3,) + w_key.shape, bf16),
            pltpu.VMEM((model, 2 * heads * width), bf16),
            pltpu.VMEM((model, heads * width), bf16),
            pltpu.VMEM(w_out.shape, bf16),
            pltpu.VMEM((3,) + w_out.shape, bf16),
            pltpu.VMEM((own_rows + context.shape[0], model), bf16),
            pltpu.VMEM((n_query, heads * width), bf16),
            pltpu.VMEM((n_sp, length, 2 * heads * width), bf16),
            pltpu.VMEM((heads * width, 2 * n_query), bf16),
            pltpu.VMEM((heads, width, 2 * n_query), f32),
            pltpu.VMEM((heads, 1, 2 * n_query), f32),
            pltpu.VMEM((heads, 1, 2 * n_query), f32),
            pltpu.VMEM((width, length), bf16),
            pltpu.VMEM((n_query, heads * width), bf16),
            pltpu.VMEM((3, own_rows, heads * width), bf16),
            dma((3,)),
            dma((3,)),
            dma((3,)),
            dma((3,)),
            dma((3,)),
            dma((3,)),
            dma((8,)),
            dma((8,)),
            dma((4,)),
            dma((n_sp, 2, n_tp)),
            dma((n_sp, n_tp)),
            dma((4,)),
            dma((4,)),
            dma((3,)),
            dma((3,)),
        ],
        compiler_params=pltpu.CompilerParams(
            collective_id=0, has_side_effects=True, vmem_limit_bytes=60 * 1024 * 1024
        ),
        name="fused",
    )(part, latent, context, norm_gain, w_query, w_key, w_value, lam, head_gain, w_out)


def on_device(
    latent, cond, cond_ctx, context, w_mod, norm_gain, w_query, w_key, w_value, lam, head_gain, w_out
):
    n_sp, n_tp = lax.axis_size("sp"), lax.axis_size("tp")
    lift = math.log(TOK_DEV / (4 * CTX_DEV))
    cond_rows = jnp.concatenate(
        [cond.astype(jnp.float32), cond_ctx.astype(jnp.float32)[None]], axis=0
    )
    partial_mod = jnp.einsum(
        "sd,jde->sje",
        jax.nn.silu(cond_rows),
        w_mod.astype(jnp.float32),
        precision=lax.Precision.HIGHEST,
    )
    columns = w_mod.shape[2]
    part = jnp.concatenate(
        [partial_mod.reshape(6, columns), jnp.zeros((2, columns), jnp.float32)], axis=0
    )
    updated = fused(
        n_sp,
        n_tp,
        lift,
        part,
        latent[0],
        context[0],
        norm_gain[None],
        w_query,
        w_key,
        w_value,
        lam,
        head_gain[:, None],
        w_out.reshape(-1, w_out.shape[2]),
    )
    return updated[None]


def solution(mesh):
    return jax.shard_map(
        on_device,
        mesh=mesh,
        in_specs=(
            P(("grp", "dp"), ("sp", "tp"), None),
            P(("grp", "dp"), "sp"),
            P("sp"),
            P(("grp", "dp"), "sp", None),
            P(None, "sp", "tp"),
            P(),
            P(None, "tp", None),
            P(None, "tp", None),
            P(None, "tp", None),
            P("tp"),
            P(),
            P("tp", None, None),
        ),
        out_specs=P(("grp", "dp"), ("sp", "tp"), None),
        check_vma=False,
    )
```

```python
import functools
import math

import jax
import jax.numpy as jnp
from jax import lax
from jax.experimental import pallas as pl
from jax.experimental.pallas import tpu as pltpu
from jax.sharding import PartitionSpec as P

TOK_DEV = 640
CTX_DEV = 32

EPSILON = 1e-06
HEAD_SCALE = 0.8
MESH = pl.DeviceIdType.MESH
QTILE = 256


def remote(src, dst, send, recv, device):
    return pltpu.make_async_remote_copy(
        src_ref=src,
        dst_ref=dst,
        send_sem=send,
        recv_sem=recv,
        device_id=device,
        device_id_type=MESH,
    )


def fused_kernel(
    n_sp, n_tp, lift,
    latent_in, cond, cond_ctx, context_in, w_mod, norm_gain, w_query, w_key, w_value, lam, head_gain, w_out, out,
    latent, context, w_mods, part, parts, mod, rows, w_raw, w_kv, w_q, w_own, w_far, tokens, queries,
    blocks, q_wide, acc, top, total, v_t, att, got,
    part_s, part_r, tp_s, tp_r, lat_s, lat_r, load_s, ring_s, ring_r, w_s, w_r, att_s, att_r,
):
    z = lax.axis_index("sp")
    x = lax.axis_index("tp")
    own_rows, n_ctx = latent.shape[0], context.shape[0]
    heads = lam.shape[0]
    width = head_gain.shape[0]
    n_query = n_tp * own_rows
    length = n_query + n_ctx
    tiles = 2 * n_query // QTILE
    steps = n_sp // 2
    starts = [0] + [n_ctx + k * own_rows for k in range(1, n_tp)]
    sizes = [n_ctx + own_rows] + [own_rows] * (n_tp - 1)

    def sp_at(offset):
        return {"sp": lax.rem(z + offset + n_sp, n_sp)}

    def tp_at(offset):
        return {"tp": lax.rem(x + offset, n_tp)}

    tp_peers = [tp_at(k) for k in (1, 2, 3)]
    right, left = tp_peers[0], tp_peers[2]
    ring_peers = [sp_at(1), sp_at(-1)]

    loads = [
        pltpu.make_async_copy(source, target, load_s.at[k])
        for k, (source, target) in enumerate(
            (
                (w_mod, w_mods),
                (latent_in, latent),
                (context_in, context),
                (w_key, w_raw.at[0]),
                (w_value, w_raw.at[1]),
                (w_query, w_raw.at[2]),
                (w_out, w_own),
            )
        )
    ]
    mod_load, latent_load, context_load, out_load = loads[0], loads[1], loads[2], loads[6]
    raw_loads = loads[3:6]
    for copy in loads:
        copy.start()
    everyone = [sp_at(k) for k in range(1, n_sp)] + tp_peers
    barrier = pltpu.get_barrier_semaphore()
    for peer in everyone:
        pl.semaphore_signal(barrier, inc=1, device_id=peer, device_id_type=MESH)

    def gated(ref):
        values = ref[...].astype(jnp.float32)
        return values * jax.nn.sigmoid(values)

    row = lax.broadcasted_iota(jnp.int32, (16, cond.shape[1]), 0)
    silu = jnp.where(row % 2 == 0, gated(cond), gated(cond_ctx))
    high = silu.astype(jnp.bfloat16)
    rest = silu - high.astype(jnp.float32)
    middle = rest.astype(jnp.bfloat16)
    low = (rest - middle.astype(jnp.float32)).astype(jnp.bfloat16)
    split = jnp.where(
        row < 2,
        high.astype(jnp.float32),
        jnp.where(
            row < 4, middle.astype(jnp.float32), jnp.where(row < 6, low.astype(jnp.float32), 0.0)
        ),
    ).astype(jnp.bfloat16)
    part[...] = jnp.zeros_like(part)
    mod_load.wait()
    for j in range(w_mods.shape[0]):
        thirds = jnp.dot(split, w_mods[j], preferred_element_type=jnp.float32)
        both = thirds[4:6] + thirds[2:4] + thirds[0:2]
        part[j : j + 1, :] = both[0:1]
        part[3 + j : 4 + j, :] = both[1:2]
    pl.semaphore_wait(barrier, len(everyone))

    part_copies = [
        remote(part, parts.at[k - 1], part_s.at[k - 1], part_r.at[k - 1], everyone[k - 1])
        for k in range(1, n_sp)
    ]
    for k in sorted(range(1, n_sp), key=lambda k: abs(k - steps)):
        part_copies[k - 1].start()
    latent_load.wait()

    half = own_rows // 2
    piece = 48

    def send_rows(k, slot, first, count, peer):
        span = pl.ds(first, count)
        return remote(latent.at[span], rows.at[slot, span], lat_s.at[k], lat_r.at[k], peer)

    to_right = [
        send_rows(0, 0, 0, half, right),
        send_rows(1, 0, half, piece, right),
        send_rows(2, 0, half + piece, half - piece, right),
    ]
    to_left = [
        send_rows(3, 1, half, half, left),
        send_rows(4, 1, 0, piece, left),
        send_rows(5, 1, piece, half - piece, left),
    ]
    first, second = pl.ds(0, half), pl.ds(half, half)
    onward_right = remote(rows.at[0, first], rows.at[2, first], lat_s.at[6], lat_r.at[6], right)
    onward_left = remote(rows.at[1, second], rows.at[2, second], lat_s.at[7], lat_r.at[7], left)
    for k in range(2):
        to_right[k].start()
        to_left[k].start()

    q_wide[...] = jnp.zeros_like(q_wide)
    acc[...] = jnp.zeros_like(acc)
    total[...] = jnp.zeros_like(total)
    top[...] = jnp.full_like(top, -1e30)
    for k in range(2):
        raw_loads[k].wait()
        for h in range(heads):
            column = (k * heads + h) * width
            w_kv[:, column : column + width] = w_raw[k, :, h, :]

    for copy in part_copies:
        copy.wait_recv()
    whole = part[...]
    for k in range(1, n_sp):
        whole = whole + parts[k - 1]
    columns = part.shape[1]

    def mod_of(owner):
        span = pl.ds(pl.multiple_of(owner * columns, columns), columns)
        return mod.at[:, span]

    mine = pl.ds(pl.multiple_of(x * columns, columns), columns)
    mod[:, mine] = whole
    tp_copies = [
        remote(mod_of(x), mod_of(x), tp_s.at[k], tp_r.at[k], tp_peers[k]) for k in range(3)
    ]
    for copy in tp_copies:
        copy.start()
    to_right[2].start()
    to_left[2].start()
    to_right[0].wait_recv()
    onward_right.start()
    to_left[0].wait_recv()
    onward_left.start()
    raw_loads[2].wait()
    for h in range(heads):
        w_q[:, h * width : (h + 1) * width] = w_raw[2, :, h, :]
    context_load.wait()
    for k in range(3):
        theirs = mod_of(lax.rem(x + n_tp - 1 - k, n_tp))
        remote(theirs, theirs, tp_s.at[k], tp_r.at[k], tp_peers[k]).wait_recv()

    def norm(source, target, count, kind):
        gain = norm_gain[...] * (1.0 + mod[kind + 1 : kind + 2, :])
        shift = mod[kind : kind + 1, :]
        group = 16

        def some(i, carry):
            span = pl.ds(pl.multiple_of(i * group, group), group)
            values = source[span, :].astype(jnp.float32)
            scale = lax.rsqrt(jnp.mean(values * values, axis=-1, keepdims=True) + EPSILON)
            spot = pl.ds(pl.multiple_of(target + i * group, group), group)
            tokens[spot, :] = (values * scale * gain + shift).astype(jnp.bfloat16)
            return carry

        lax.fori_loop(0, count // group, some, 0, unroll=2)

    def ring_copy(slot, target, d, c):
        span = pl.ds(starts[c], sizes[c])
        return remote(
            blocks.at[slot, span],
            blocks.at[target, span],
            ring_s.at[slot, d, c],
            ring_r.at[target, c],
            ring_peers[d],
        )

    def project(c):
        span = slice(starts[c], starts[c] + sizes[c])
        blocks[0, span, :] = jnp.dot(
            tokens[: sizes[c], :], w_kv[...], preferred_element_type=jnp.float32
        ).astype(jnp.bfloat16)
        queries[c * own_rows : (c + 1) * own_rows, :] = jnp.dot(
            tokens[:own_rows, :], w_q[...], preferred_element_type=jnp.float32
        ).astype(jnp.bfloat16)
        for d in range(2):
            ring_copy(0, 1 + d, d, c).start()

    norm(latent, 0, own_rows, 0)
    norm(context, own_rows, n_ctx, 3)
    project(0)
    for k in (1, 2):
        to_right[k].wait_recv()
    norm(rows.at[0], 0, own_rows, 0)
    project(1)
    for k in (1, 2):
        to_left[k].wait_recv()
    norm(rows.at[1], 0, own_rows, 0)
    project(2)
    onward_right.wait_recv()
    onward_left.wait_recv()
    norm(rows.at[2], 0, own_rows, 0)
    project(3)

    w_rows = w_own.shape[0]
    upper, lower = pl.ds(0, w_rows // 2), pl.ds(w_rows // 2, w_rows // 2)
    w_right = remote(w_own, w_far.at[0], w_s.at[0], w_r.at[0], right)
    w_left = remote(w_own, w_far.at[2], w_s.at[1], w_r.at[1], left)
    w_right_on = remote(w_far.at[0, upper], w_far.at[1, upper], w_s.at[2], w_r.at[2], right)
    w_left_on = remote(w_far.at[2, lower], w_far.at[1, lower], w_s.at[3], w_r.at[3], left)
    out_load.wait()
    w_right.start()
    w_left.start()

    half_width = width // 2
    for h in range(heads):
        for m in range(2):
            span = slice(h * width + m * half_width, h * width + (m + 1) * half_width)
            q_wide[span, m * n_query : (m + 1) * n_query] = queries[:, span].T * jnp.bfloat16(
                half_width ** (-0.5)
            )

    def fold(block, after=None):
        def head(h, carry):
            base = pl.multiple_of(h * width, width)
            keys = block[:, pl.ds(base, width)]
            v_t[...] = block[:, pl.ds(pl.multiple_of(heads * width + base, width), width)].T
            for j in range(tiles):
                columns = slice(j * QTILE, (j + 1) * QTILE)
                scores = jnp.dot(
                    keys, q_wide[pl.ds(base, width), columns], preferred_element_type=jnp.float32
                )
                scores = jnp.concatenate(
                    [
                        scores[:own_rows],
                        scores[own_rows : own_rows + n_ctx] + lift,
                        scores[own_rows + n_ctx :],
                    ],
                    axis=0,
                )
                old = top[h, :, columns]
                new = jnp.maximum(old, jnp.max(scores, axis=0, keepdims=True))
                weights = jnp.exp(scores - new)
                rescale = jnp.exp(old - new)
                top[h, :, columns] = new
                total[h, :, columns] = total[h, :, columns] * rescale + jnp.sum(
                    weights, axis=0, keepdims=True
                )
                acc[h, :, columns] = acc[h, :, columns] * rescale + jnp.dot(
                    v_t[...], weights.astype(jnp.bfloat16), preferred_element_type=jnp.float32
                )
            if after is not None:
                after(h, base)
            return carry

        lax.fori_loop(0, heads, head, 0)

    def forward(s, d, c):
        slot = 2 * s - 1 + d
        return ring_copy(slot, jnp.minimum(slot + 2, 2 * steps - 1), d, c)

    def arrived(slot, c):
        ring_copy(slot, slot, 0, c).wait_recv()

    def always(d, c):
        return (c < n_tp // 2) == (d == 0)

    def half_step(u, carry):
        s = u // 2 + 1
        for phase in range(2):

            @pl.when(jnp.logical_and(u < 2 * steps - 2, u % 2 == phase))
            def _():
                for c in (2 * phase, 2 * phase + 1):
                    for d in range(2):
                        arrived(2 * s - 1 + d, c)
                        if always(d, c):
                            forward(s, d, c).start()
                        else:

                            @pl.when(s < steps - 1)
                            def _():
                                forward(s, d, c).start()

        @pl.when(u == 2 * steps - 2)
        def _():
            arrived(2 * steps - 1, 0)
            arrived(2 * steps - 1, 2)

        @pl.when(u == 6)
        def _():
            w_right.wait_recv()
            w_right_on.start()
            w_left.wait_recv()
            w_left_on.start()

        fold(blocks.at[u])
        return carry

    lax.fori_loop(0, 2 * steps - 1, half_step, 0)

    slot_of = {1: 2, 2: 3, 3: 1}

    def send_head(h, base, k):
        span = pl.ds(slot_of[k] * own_rows, own_rows)
        lanes = pl.ds(base, width)
        return remote(
            att.at[span, lanes],
            got.at[k - 1, :, lanes],
            att_s.at[k - 1, h],
            att_r.at[k - 1, h],
            tp_peers[k - 1],
        )

    def finish(h, base):
        one = acc[h, :, :n_query] / total[h, :, :n_query]
        two = acc[h, :, n_query:] / total[h, :, n_query:]
        differ = one - lam[h] * two
        scale = lax.rsqrt(jnp.mean(differ * differ, axis=0, keepdims=True) + EPSILON)
        normed = differ * scale * head_gain[...] * HEAD_SCALE
        att[:, pl.ds(base, width)] = normed.T.astype(jnp.bfloat16)
        for k in (2, 1, 3):
            send_head(h, base, k).start()

    arrived(2 * steps - 1, 1)
    arrived(2 * steps - 1, 3)
    fold(blocks.at[2 * steps - 1], finish)
    sends = [send_head(h, h * width, k) for h in range(heads) for k in (2, 1, 3)]
    w_right_on.wait_recv()
    w_left_on.wait_recv()
    for copy in sends:
        copy.wait_recv()
    n_columns = latent.shape[1]
    step = 512
    for j in range(n_columns // step):
        columns = slice(j * step, (j + 1) * step)
        mixed = jnp.dot(att[:own_rows, :], w_own[:, columns], preferred_element_type=jnp.float32)
        for k in range(3):
            mixed += jnp.dot(got[k], w_far[k, :, columns], preferred_element_type=jnp.float32)
        out[:, columns] = (
            latent[:, columns].astype(jnp.float32) + mod[2:3, columns] * mixed
        ).astype(out.dtype)

    for copy in part_copies + tp_copies + to_right + to_left + sends:
        copy.wait_send()
    for copy in [onward_right, onward_left, w_right, w_left, w_right_on, w_left_on]:
        copy.wait_send()
    for c in range(n_tp):
        for d in range(2):
            ring_copy(0, 1 + d, d, c).wait_send()

    def drain(s, carry):
        for c in range(n_tp):
            for d in range(2):
                if always(d, c):
                    forward(s, d, c).wait_send()
                else:

                    @pl.when(s < steps - 1)
                    def _():
                        forward(s, d, c).wait_send()

        return carry

    lax.fori_loop(1, steps, drain, 0)


def fused(n_sp, n_tp, lift, latent, cond, cond_ctx, context, w_mod, norm_gain, w_query, w_key, w_value, lam, head_gain, w_out):
    dma = pltpu.SemaphoreType.DMA
    vmem = pl.BlockSpec(memory_space=pltpu.VMEM)
    anywhere = pl.BlockSpec(memory_space=pl.ANY)
    heads, width = lam.shape[0], head_gain.shape[0]
    own_rows, model = latent.shape
    n_query = n_tp * own_rows
    length = n_query + context.shape[0]
    bf16, f32 = jnp.bfloat16, jnp.float32
    return pl.pallas_call(
        functools.partial(fused_kernel, n_sp, n_tp, lift),
        out_shape=jax.ShapeDtypeStruct(latent.shape, latent.dtype),
        in_specs=[anywhere, vmem, vmem, anywhere, anywhere, vmem]
        + [anywhere] * 3
        + [pl.BlockSpec(memory_space=pltpu.SMEM), vmem, anywhere],
        out_specs=vmem,
        scratch_shapes=[
            pltpu.VMEM(latent.shape, bf16),
            pltpu.VMEM(context.shape, bf16),
            pltpu.VMEM(w_mod.shape, bf16),
            pltpu.VMEM((8, w_mod.shape[2]), f32),
            pltpu.VMEM((n_sp - 1, 8, w_mod.shape[2]), f32),
            pltpu.VMEM((8, model), f32),
            pltpu.VMEM((3, own_rows, model), bf16),
            pltpu.VMEM((3,) + w_key.shape, bf16),
            pltpu.VMEM((model, 2 * heads * width), bf16),
            pltpu.VMEM((model, heads * width), bf16),
            pltpu.VMEM(w_out.shape, bf16),
            pltpu.VMEM((3,) + w_out.shape, bf16),
            pltpu.VMEM((own_rows + context.shape[0], model), bf16),
            pltpu.VMEM((n_query, heads * width), bf16),
            pltpu.VMEM((n_sp, length, 2 * heads * width), bf16),
            pltpu.VMEM((heads * width, 2 * n_query), bf16),
            pltpu.VMEM((heads, width, 2 * n_query), f32),
            pltpu.VMEM((heads, 1, 2 * n_query), f32),
            pltpu.VMEM((heads, 1, 2 * n_query), f32),
            pltpu.VMEM((width, length), bf16),
            pltpu.VMEM((n_query, heads * width), bf16),
            pltpu.VMEM((3, own_rows, heads * width), bf16),
            dma((n_sp - 1,)),
            dma((n_sp - 1,)),
            dma((3,)),
            dma((3,)),
            dma((8,)),
            dma((8,)),
            dma((7,)),
            dma((n_sp, 2, n_tp)),
            dma((n_sp, n_tp)),
            dma((4,)),
            dma((4,)),
            dma((3, heads)),
            dma((3, heads)),
        ],
        compiler_params=pltpu.CompilerParams(
            collective_id=0, has_side_effects=True, vmem_limit_bytes=60 * 1024 * 1024
        ),
        name="fused",
    )(latent, cond, cond_ctx, context, w_mod, norm_gain, w_query, w_key, w_value, lam, head_gain, w_out)


def on_device(
    latent, cond, cond_ctx, context, w_mod, norm_gain, w_query, w_key, w_value, lam, head_gain, w_out
):
    n_sp, n_tp = lax.axis_size("sp"), lax.axis_size("tp")
    lift = math.log(TOK_DEV / (4 * CTX_DEV))
    updated = fused(
        n_sp,
        n_tp,
        lift,
        latent[0],
        cond,
        cond_ctx[None],
        context[0],
        w_mod,
        norm_gain[None],
        w_query,
        w_key,
        w_value,
        lam,
        head_gain[:, None],
        w_out.reshape(-1, w_out.shape[2]),
    )
    return updated[None]


def solution(mesh):
    return jax.shard_map(
        on_device,
        mesh=mesh,
        in_specs=(
            P(("grp", "dp"), ("sp", "tp"), None),
            P(("grp", "dp"), "sp"),
            P("sp"),
            P(("grp", "dp"), "sp", None),
            P(None, "sp", "tp"),
            P(),
            P(None, "tp", None),
            P(None, "tp", None),
            P(None, "tp", None),
            P("tp"),
            P(),
            P("tp", None, None),
        ),
        out_specs=P(("grp", "dp"), ("sp", "tp"), None),
        check_vma=False,
    )
```

```python
import functools
import math

import jax
import jax.numpy as jnp
from jax import lax
from jax.experimental import pallas as pl
from jax.experimental.pallas import tpu as pltpu
from jax.sharding import PartitionSpec as P

TOK_DEV = 640
CTX_DEV = 32

EPSILON = 1e-06
HEAD_SCALE = 0.8
MESH = pl.DeviceIdType.MESH
QTILE = 256


def remote(src, dst, send, recv, device):
    return pltpu.make_async_remote_copy(
        src_ref=src,
        dst_ref=dst,
        send_sem=send,
        recv_sem=recv,
        device_id=device,
        device_id_type=MESH,
    )


def fused_kernel(
    n_sp, n_tp, lift,
    latent_in, cond, cond_ctx, context_in, w_mod, norm_gain, w_query, w_key, w_value, lam, head_gain, w_out, out,
    latent, context, w_mods, part, parts, gate, gates, mod, whole_gate, rows, w_raw, w_kv, w_q, w_own, w_far, tokens, queries,
    blocks, q_wide, acc, top, total, v_t, att, got,
    part_s, part_r, gate_s, gate_r, tp_s, tp_r, gate_tp_s, gate_tp_r, lat_s, lat_r, load_s, ring_s, ring_r, w_s, w_r, att_s, att_r,
):
    z = lax.axis_index("sp")
    x = lax.axis_index("tp")
    own_rows, n_ctx = latent.shape[0], context.shape[0]
    heads = lam.shape[0]
    width = head_gain.shape[0]
    n_query = n_tp * own_rows
    length = n_query + n_ctx
    tiles = 2 * n_query // QTILE
    steps = n_sp // 2
    starts = [0] + [n_ctx + k * own_rows for k in range(1, n_tp)]
    sizes = [n_ctx + own_rows] + [own_rows] * (n_tp - 1)

    def sp_at(offset):
        return {"sp": lax.rem(z + offset + n_sp, n_sp)}

    def tp_at(offset):
        return {"tp": lax.rem(x + offset, n_tp)}

    tp_peers = [tp_at(k) for k in (1, 2, 3)]
    right, left = tp_peers[0], tp_peers[2]
    ring_peers = [sp_at(1), sp_at(-1)]

    loads = [
        pltpu.make_async_copy(source, target, load_s.at[k])
        for k, (source, target) in enumerate(
            (
                (w_mod, w_mods),
                (latent_in, latent),
                (context_in, context),
                (w_key, w_raw.at[0]),
                (w_value, w_raw.at[1]),
                (w_query, w_raw.at[2]),
                (w_out, w_own),
            )
        )
    ]
    mod_load, latent_load, context_load, out_load = loads[0], loads[1], loads[2], loads[6]
    raw_loads = loads[3:6]
    for copy in loads:
        copy.start()
    everyone = [sp_at(k) for k in range(1, n_sp)] + tp_peers
    barrier = pltpu.get_barrier_semaphore()
    for peer in everyone:
        pl.semaphore_signal(barrier, inc=1, device_id=peer, device_id_type=MESH)

    def gated(ref):
        values = ref[...].astype(jnp.float32)
        return values * jax.nn.sigmoid(values)

    row = lax.broadcasted_iota(jnp.int32, (16, cond.shape[1]), 0)
    silu = jnp.where(row % 2 == 0, gated(cond), gated(cond_ctx))
    high = silu.astype(jnp.bfloat16)
    rest = silu - high.astype(jnp.float32)
    middle = rest.astype(jnp.bfloat16)
    low = (rest - middle.astype(jnp.float32)).astype(jnp.bfloat16)
    split = jnp.where(
        row < 2,
        high.astype(jnp.float32),
        jnp.where(
            row < 4, middle.astype(jnp.float32), jnp.where(row < 6, low.astype(jnp.float32), 0.0)
        ),
    ).astype(jnp.bfloat16)
    columns = w_mods.shape[2]
    middle_column = columns // 2
    mod_load.wait()
    for j in range(w_mods.shape[0]):
        thirds = jnp.dot(split, w_mods[j], preferred_element_type=jnp.float32)
        both = thirds[4:6] + thirds[2:4] + thirds[0:2]
        if j == 2:
            gate[...] = both[0:1]
        else:
            for of_ctx in range(2):
                at = 2 * of_ctx + j
                part[at : at + 1, :] = both[of_ctx : of_ctx + 1, :middle_column]
                part[4 + at : 5 + at, :] = both[of_ctx : of_ctx + 1, middle_column:]
    pl.semaphore_wait(barrier, len(everyone))

    far_first = sorted(range(n_sp - 1), key=lambda k: abs(k + 1 - steps))
    part_copies = [remote(part, parts.at[k], part_s, part_r, everyone[k]) for k in far_first]
    gate_copies = [remote(gate, gates.at[k], gate_s, gate_r, everyone[k]) for k in far_first]
    all_parts = remote(parts, parts, part_s, part_r, everyone[0])
    all_gates = remote(gates, gates, gate_s, gate_r, everyone[0])
    for copy in part_copies + gate_copies:
        copy.start()
    latent_load.wait()

    half = own_rows // 2
    piece = 48

    def send_rows(k, slot, first, count, peer):
        span = pl.ds(first, count)
        return remote(latent.at[span], rows.at[slot, span], lat_s.at[k], lat_r.at[k], peer)

    to_right = [
        send_rows(0, 0, 0, half, right),
        send_rows(1, 0, half, piece, right),
        send_rows(2, 0, half + piece, half - piece, right),
    ]
    to_left = [
        send_rows(3, 1, half, half, left),
        send_rows(4, 1, 0, piece, left),
        send_rows(5, 1, piece, half - piece, left),
    ]
    first, second = pl.ds(0, half), pl.ds(half, half)
    onward_right = remote(rows.at[0, first], rows.at[2, first], lat_s.at[6], lat_r.at[6], right)
    onward_left = remote(rows.at[1, second], rows.at[2, second], lat_s.at[7], lat_r.at[7], left)
    for k in range(2):
        to_right[k].start()
        to_left[k].start()

    q_wide[...] = jnp.zeros_like(q_wide)
    acc[...] = jnp.zeros_like(acc)
    total[...] = jnp.zeros_like(total)
    top[...] = jnp.full_like(top, -1e30)
    for k in range(2):
        raw_loads[k].wait()
        for h in range(heads):
            column = (k * heads + h) * width
            w_kv[:, column : column + width] = w_raw[k, :, h, :]

    all_parts.wait_recv()
    whole = part[...]
    for k in range(n_sp - 1):
        whole = whole + parts[k]

    def mod_of(owner):
        span = pl.ds(pl.multiple_of(owner * columns, columns), columns)
        return mod.at[:, span]

    mine = pl.ds(pl.multiple_of(x * columns, columns), columns)
    at_middle = pl.multiple_of(x * columns + middle_column, middle_column)
    mod[:, pl.ds(pl.multiple_of(x * columns, columns), middle_column)] = whole[:4]
    mod[:, pl.ds(at_middle, middle_column)] = whole[4:]
    tp_copies = [
        remote(mod_of(x), mod_of(x), tp_s.at[k], tp_r.at[k], tp_peers[k]) for k in range(3)
    ]
    for copy in tp_copies:
        copy.start()
    to_right[2].start()
    to_left[2].start()
    to_right[0].wait_recv()
    onward_right.start()
    to_left[0].wait_recv()
    onward_left.start()
    raw_loads[2].wait()
    for h in range(heads):
        w_q[:, h * width : (h + 1) * width] = w_raw[2, :, h, :]
    context_load.wait()
    for k in range(3):
        theirs = mod_of(lax.rem(x + n_tp - 1 - k, n_tp))
        remote(theirs, theirs, tp_s.at[k], tp_r.at[k], tp_peers[k]).wait_recv()

    def norm(source, target, count, kind):
        gain = norm_gain[...] * (1.0 + mod[kind + 1 : kind + 2, :])
        shift = mod[kind : kind + 1, :]
        group = 16

        def some(i, carry):
            span = pl.ds(pl.multiple_of(i * group, group), group)
            values = source[span, :].astype(jnp.float32)
            scale = lax.rsqrt(jnp.mean(values * values, axis=-1, keepdims=True) + EPSILON)
            spot = pl.ds(pl.multiple_of(target + i * group, group), group)
            tokens[spot, :] = (values * scale * gain + shift).astype(jnp.bfloat16)
            return carry

        lax.fori_loop(0, count // group, some, 0, unroll=2)

    def ring_copy(slot, target, d, c, turn=0):
        span = pl.ds(starts[c], sizes[c])
        return remote(
            blocks.at[slot, span],
            blocks.at[target, span],
            ring_s.at[turn, d, c],
            ring_r.at[target, c],
            ring_peers[d],
        )

    def project(c):
        span = slice(starts[c], starts[c] + sizes[c])
        blocks[0, span, :] = jnp.dot(
            tokens[: sizes[c], :], w_kv[...], preferred_element_type=jnp.float32
        ).astype(jnp.bfloat16)
        queries[c * own_rows : (c + 1) * own_rows, :] = jnp.dot(
            tokens[:own_rows, :], w_q[...], preferred_element_type=jnp.float32
        ).astype(jnp.bfloat16)
        for d in range(2):
            ring_copy(0, 1 + d, d, c).start()

    norm(latent, 0, own_rows, 0)
    norm(context, own_rows, n_ctx, 2)
    project(0)
    for k in (1, 2):
        to_right[k].wait_recv()
    norm(rows.at[0], 0, own_rows, 0)
    project(1)
    for k in (1, 2):
        to_left[k].wait_recv()
    norm(rows.at[1], 0, own_rows, 0)
    project(2)
    onward_right.wait_recv()
    onward_left.wait_recv()
    norm(rows.at[2], 0, own_rows, 0)
    project(3)

    all_gates.wait_recv()
    gate_sum = gate[...]
    for k in range(n_sp - 1):
        gate_sum = gate_sum + gates[k]
    whole_gate[:, mine] = gate_sum

    def gate_of(owner):
        return whole_gate.at[:, pl.ds(pl.multiple_of(owner * columns, columns), columns)]

    gate_tp_copies = [
        remote(gate_of(x), gate_of(x), gate_tp_s.at[k], gate_tp_r.at[k], tp_peers[k])
        for k in range(3)
    ]
    for copy in gate_tp_copies:
        copy.start()

    w_rows = w_own.shape[0]
    upper, lower = pl.ds(0, w_rows // 2), pl.ds(w_rows // 2, w_rows // 2)
    w_right = remote(w_own, w_far.at[0], w_s.at[0], w_r.at[0], right)
    w_left = remote(w_own, w_far.at[2], w_s.at[1], w_r.at[1], left)
    w_right_on = remote(w_far.at[0, upper], w_far.at[1, upper], w_s.at[2], w_r.at[2], right)
    w_left_on = remote(w_far.at[2, lower], w_far.at[1, lower], w_s.at[3], w_r.at[3], left)
    out_load.wait()
    w_right.start()
    w_left.start()

    half_width = width // 2
    for h in range(heads):
        for m in range(2):
            span = slice(h * width + m * half_width, h * width + (m + 1) * half_width)
            q_wide[span, m * n_query : (m + 1) * n_query] = queries[:, span].T * jnp.bfloat16(
                half_width ** (-0.5)
            )

    half_row = starts[n_tp // 2]
    spans = [(0, half_row), (half_row, length)]

    def fold(block, phase, after=None):
        begin, end = spans[phase]
        count = end - begin

        def head(h, carry):
            base = pl.multiple_of(h * width, width)
            keys = block[begin:end, pl.ds(base, width)]
            v_t[:, :count] = block[begin:end, pl.ds(pl.multiple_of(heads * width + base, width), width)].T
            for j in range(tiles):
                columns = slice(j * QTILE, (j + 1) * QTILE)
                scores = jnp.dot(
                    keys, q_wide[pl.ds(base, width), columns], preferred_element_type=jnp.float32
                )
                if phase == 0:
                    scores = jnp.concatenate(
                        [
                            scores[:own_rows],
                            scores[own_rows : own_rows + n_ctx] + lift,
                            scores[own_rows + n_ctx :],
                        ],
                        axis=0,
                    )
                old = top[h, :, columns]
                new = jnp.maximum(old, jnp.max(scores, axis=0, keepdims=True))
                weights = jnp.exp(scores - new)
                rescale = jnp.exp(old - new)
                top[h, :, columns] = new
                total[h, :, columns] = total[h, :, columns] * rescale + jnp.sum(
                    weights, axis=0, keepdims=True
                )
                acc[h, :, columns] = acc[h, :, columns] * rescale + jnp.dot(
                    v_t[:, :count], weights.astype(jnp.bfloat16), preferred_element_type=jnp.float32
                )
            if after is not None:
                after(h, base)
            return carry

        lax.fori_loop(0, heads, head, 0)

    def forward(s, d, c):
        slot = 2 * s - 1 + d
        return ring_copy(slot, jnp.minimum(slot + 2, 2 * steps - 1), d, c, lax.rem(s, 2))

    def send_on(s, d, c):
        @pl.when(s >= 2)
        def _():
            ring_copy(0, 1 + d, d, c, lax.rem(s, 2)).wait_send()

        forward(s, d, c).start()

    def arrived(slot, c):
        ring_copy(slot, slot, 0, c).wait_recv()

    def always(d, c):
        return c % 2 == d

    def half_step(u, carry):
        s = u // 2 + 1
        for phase in range(2):

            @pl.when(jnp.logical_and(u < 2 * steps - 2, u % 2 == phase))
            def _():
                for c in (2 * phase, 2 * phase + 1):
                    for d in range(2):
                        arrived(2 * s - 1 + d, c)
                        if always(d, c):
                            send_on(s, d, c)
                        else:

                            @pl.when(s < steps - 1)
                            def _():
                                send_on(s, d, c)

        @pl.when(u == 2 * steps - 2)
        def _():
            arrived(2 * steps - 1, 0)
            arrived(2 * steps - 1, 1)

        @pl.when(u == 6)
        def _():
            w_right.wait_recv()
            w_right_on.start()
            w_left.wait_recv()
            w_left_on.start()

        for phase in range(2):

            @pl.when(u % 2 == phase)
            def _():
                def one_half(k, carry):
                    wanted = jnp.logical_or(
                        k == 1,
                        jnp.logical_or(
                            jnp.logical_and(k == 0, s == 1), jnp.logical_and(k == 2, s < steps)
                        ),
                    )

                    @pl.when(wanted)
                    def _():
                        fold(blocks.at[2 * s - 2 + k], phase)

                    return carry

                lax.fori_loop(0, 3, one_half, 0)

        return carry

    lax.fori_loop(0, 2 * steps - 1, half_step, 0)

    slot_of = {1: 2, 2: 3, 3: 1}

    def send_head(h, base, k):
        span = pl.ds(slot_of[k] * own_rows, own_rows)
        lanes = pl.ds(base, width)
        return remote(
            att.at[span, lanes],
            got.at[k - 1, :, lanes],
            att_s.at[k - 1, h],
            att_r.at[k - 1, h],
            tp_peers[k - 1],
        )

    def finish(h, base):
        one = acc[h, :, :n_query] / total[h, :, :n_query]
        two = acc[h, :, n_query:] / total[h, :, n_query:]
        differ = one - lam[h] * two
        scale = lax.rsqrt(jnp.mean(differ * differ, axis=0, keepdims=True) + EPSILON)
        normed = differ * scale * head_gain[...] * HEAD_SCALE
        att[:, pl.ds(base, width)] = normed.T.astype(jnp.bfloat16)
        for k in (2, 1, 3):
            send_head(h, base, k).start()

    arrived(2 * steps - 1, 2)
    arrived(2 * steps - 1, 3)
    fold(blocks.at[2 * steps - 1], 1, finish)
    sends = [send_head(h, h * width, k) for h in range(heads) for k in (2, 1, 3)]
    w_right_on.wait_recv()
    w_left_on.wait_recv()
    for copy in sends:
        copy.wait_recv()
    for k in range(3):
        theirs = gate_of(lax.rem(x + n_tp - 1 - k, n_tp))
        remote(theirs, theirs, gate_tp_s.at[k], gate_tp_r.at[k], tp_peers[k]).wait_recv()
    n_columns = latent.shape[1]
    step = 512
    for j in range(n_columns // step):
        columns = slice(j * step, (j + 1) * step)
        mixed = jnp.dot(att[:own_rows, :], w_own[:, columns], preferred_element_type=jnp.float32)
        for k in range(3):
            mixed += jnp.dot(got[k], w_far[k, :, columns], preferred_element_type=jnp.float32)
        out[:, columns] = (
            latent[:, columns].astype(jnp.float32) + whole_gate[:, columns] * mixed
        ).astype(out.dtype)

    all_parts.wait_send()
    all_gates.wait_send()
    for copy in gate_tp_copies + tp_copies + to_right + to_left + sends:
        copy.wait_send()
    for copy in [onward_right, onward_left, w_right, w_left, w_right_on, w_left_on]:
        copy.wait_send()
    for turn in range(2):
        for c in range(n_tp):
            for d in range(2):
                ring_copy(0, 1 + d, d, c, turn).wait_send()


def fused(n_sp, n_tp, lift, latent, cond, cond_ctx, context, w_mod, norm_gain, w_query, w_key, w_value, lam, head_gain, w_out):
    dma = pltpu.SemaphoreType.DMA
    vmem = pl.BlockSpec(memory_space=pltpu.VMEM)
    anywhere = pl.BlockSpec(memory_space=pl.ANY)
    heads, width = lam.shape[0], head_gain.shape[0]
    own_rows, model = latent.shape
    n_query = n_tp * own_rows
    length = n_query + context.shape[0]
    bf16, f32 = jnp.bfloat16, jnp.float32
    return pl.pallas_call(
        functools.partial(fused_kernel, n_sp, n_tp, lift),
        out_shape=jax.ShapeDtypeStruct(latent.shape, latent.dtype),
        in_specs=[anywhere, vmem, vmem, anywhere, anywhere, vmem]
        + [anywhere] * 3
        + [pl.BlockSpec(memory_space=pltpu.SMEM), vmem, anywhere],
        out_specs=vmem,
        scratch_shapes=[
            pltpu.VMEM(latent.shape, bf16),
            pltpu.VMEM(context.shape, bf16),
            pltpu.VMEM(w_mod.shape, bf16),
            pltpu.VMEM((8, w_mod.shape[2] // 2), f32),
            pltpu.VMEM((n_sp - 1, 8, w_mod.shape[2] // 2), f32),
            pltpu.VMEM((1, w_mod.shape[2]), f32),
            pltpu.VMEM((n_sp - 1, 1, w_mod.shape[2]), f32),
            pltpu.VMEM((4, model), f32),
            pltpu.VMEM((1, model), f32),
            pltpu.VMEM((3, own_rows, model), bf16),
            pltpu.VMEM((3,) + w_key.shape, bf16),
            pltpu.VMEM((model, 2 * heads * width), bf16),
            pltpu.VMEM((model, heads * width), bf16),
            pltpu.VMEM(w_out.shape, bf16),
            pltpu.VMEM((3,) + w_out.shape, bf16),
            pltpu.VMEM((own_rows + context.shape[0], model), bf16),
            pltpu.VMEM((n_query, heads * width), bf16),
            pltpu.VMEM((n_sp, length, 2 * heads * width), bf16),
            pltpu.VMEM((heads * width, 2 * n_query), bf16),
            pltpu.VMEM((heads, width, 2 * n_query), f32),
            pltpu.VMEM((heads, 1, 2 * n_query), f32),
            pltpu.VMEM((heads, 1, 2 * n_query), f32),
            pltpu.VMEM((width, 512), bf16),
            pltpu.VMEM((n_query, heads * width), bf16),
            pltpu.VMEM((3, own_rows, heads * width), bf16),
            dma,
            dma,
            dma,
            dma,
            dma((3,)),
            dma((3,)),
            dma((3,)),
            dma((3,)),
            dma((8,)),
            dma((8,)),
            dma((7,)),
            dma((2, 2, n_tp)),
            dma((n_sp, n_tp)),
            dma((4,)),
            dma((4,)),
            dma((3, heads)),
            dma((3, heads)),
        ],
        compiler_params=pltpu.CompilerParams(
            collective_id=0, has_side_effects=True, vmem_limit_bytes=60 * 1024 * 1024
        ),
        name="fused",
    )(latent, cond, cond_ctx, context, w_mod, norm_gain, w_query, w_key, w_value, lam, head_gain, w_out)


def on_device(
    latent, cond, cond_ctx, context, w_mod, norm_gain, w_query, w_key, w_value, lam, head_gain, w_out
):
    n_sp, n_tp = lax.axis_size("sp"), lax.axis_size("tp")
    lift = math.log(TOK_DEV / (4 * CTX_DEV))
    updated = fused(
        n_sp,
        n_tp,
        lift,
        latent[0],
        cond,
        cond_ctx[None],
        context[0],
        w_mod,
        norm_gain[None],
        w_query,
        w_key,
        w_value,
        lam,
        head_gain[:, None],
        w_out.reshape(-1, w_out.shape[2]),
    )
    return updated[None]


def solution(mesh):
    return jax.shard_map(
        on_device,
        mesh=mesh,
        in_specs=(
            P(("grp", "dp"), ("sp", "tp"), None),
            P(("grp", "dp"), "sp"),
            P("sp"),
            P(("grp", "dp"), "sp", None),
            P(None, "sp", "tp"),
            P(),
            P(None, "tp", None),
            P(None, "tp", None),
            P(None, "tp", None),
            P("tp"),
            P(),
            P("tp", None, None),
        ),
        out_specs=P(("grp", "dp"), ("sp", "tp"), None),
        check_vma=False,
    )
```
